32 devices in a mesh: sp: 16 (over z, y, x), tp: 2 (over core).
Axes of the slice: x: 2, y: 2, z: 4, core: 2. Of those that a mesh axis runs over, the one named last changes fastest.
Arguments:
- tokens: bfloat16 [6144, 2048], P(('sp', 'tp')), may hold values from -6 to 6
- norm_gain: float32 [2048], replicated, may hold values from 0.1 to 1.9
- w_query: bfloat16 [2048, 1024], P(None, 'tp'), may hold values from -0.125 to 0.125
- w_key: bfloat16 [2048, 1024], P(None, 'tp'), may hold values from -0.125 to 0.125
- w_value: bfloat16 [2048, 2048], P(None, 'tp'), may hold values from -0.125 to 0.125
- w_ogate: bfloat16 [2048, 2048], P(None, 'tp'), may hold values from -0.125 to 0.125
- w_igate: bfloat16 [2048, 8], replicated, may hold values from -0.125 to 0.125
- w_fgate: bfloat16 [2048, 8], replicated, may hold values from -0.125 to 0.125
- conv_query: bfloat16 [4, 1024], replicated, may hold values from -3 to 3
- conv_key: bfloat16 [4, 1024], replicated, may hold values from -3 to 3
- gate_offset: float32 [2, 48, 8], P(None, 'sp', 'tp'), may hold values from -60 to 140, as said below
- head_gain: float32 [2048], replicated, may hold values from 0.1 to 1.9
- w_out: bfloat16 [2048, 2048], P('tp'), may hold values from -0.125 to 0.125
Outputs:
- mixed: bfloat16 [6144, 2048], P(('sp', 'tp'))
The draws below stay inside these ranges and needn't reach their ends.
Inputs may be any that keep to these rules, and one draw needn't show every extreme that they name: `gate_offset`: row 0 is added to the input gate's pre-activation and row 1 to the forget gate's; each entry holds for one block of 128 positions and one head.
All inputs are finite; a program needn't handle non-finite values.
Results may differ from the reference program's by a relative error of at most 0.011.
Values may be sent and summed in bfloat16 or wider, within the bound.
A program may use at most 128 MiB of HBM per device.

```python
import math
import jax
import jax.numpy as jnp
from jax import lax

D = 2048
HEADS = 8
DQK = 128
DV = 256
CONV = 4
SPAN = 128
TOKENS = 6144
SPANS = 48


def draw_gate_offset(key, part):
    seeds = jax.random.split(jax.random.fold_in(key, 7), 4)
    ranking = jax.random.permutation(seeds[0], HEADS)
    slow_heads = ranking < HEADS // 2
    inputs = jax.random.uniform(seeds[3], (SPANS, HEADS), jnp.float32, -3.0, 1.0)
    fast_level = jax.random.uniform(seeds[1], (HEADS,), jnp.float32, 3.5, 4.5)
    level_base = jnp.where(slow_heads, math.log(TOKENS) + 1.0, fast_level)
    wiggle = jax.random.uniform(seeds[2], (SPANS, HEADS), jnp.float32, -0.7, 0.7)
    return jnp.stack([inputs, level_base[None, :] + wiggle]).astype(jnp.float32)


def level_of(rng, extent, pieces, least, largest):
    loudness, own = 1.0, jax.random.fold_in(rng, 6)
    for dim, shards_of in pieces:
        heights = jnp.exp(jax.random.uniform(jax.random.fold_in(own, dim), (shards_of,), jnp.float32, least / len(pieces), largest / len(pieces)))
        loudness = loudness * jnp.repeat(heights, extent[dim] // shards_of).reshape([-1 if axis == dim else 1 for axis in range(len(extent))])
    return loudness


def noise(rng, dims, scale, bound, pieces=(), held_as=jnp.bfloat16):
    gain = level_of(rng, dims, pieces, -0.22, 0.18) if pieces else 1.0
    drawn = jax.random.normal(rng, dims, jnp.float32) * scale * gain
    return jnp.minimum(jnp.maximum(drawn, -bound), bound).astype(held_as)


def setup_inputs(seed: int = 0) -> dict:
    key_of = jax.random.split(jax.random.key(seed), 14)
    tokens = noise(key_of[0], (TOKENS, D), 1.0, 6.0, ((0, 32),))
    norm_gain = jnp.clip(1.0 + 0.18 * jax.random.normal(key_of[1], (D,), jnp.float32), 0.1, 1.9)
    w_query = noise(key_of[2], (D, HEADS * DQK), D ** -0.5, 0.125, ((1, 2),))
    w_key = noise(key_of[3], (D, HEADS * DQK), D ** -0.5, 0.125, ((1, 2),))
    w_value = noise(key_of[4], (D, HEADS * DV), D ** -0.5, 0.125, ((1, 2),))
    w_ogate = noise(key_of[5], (D, HEADS * DV), D ** -0.5, 0.125, ((1, 2),))
    w_igate = noise(key_of[6], (D, HEADS), D ** -0.5, 0.125)
    w_fgate = noise(key_of[7], (D, HEADS), D ** -0.5, 0.125)
    conv_query = noise(key_of[8], (CONV, HEADS * DQK), CONV ** -0.5, 3.0)
    conv_key = noise(key_of[9], (CONV, HEADS * DQK), CONV ** -0.5, 3.0)
    gate_offset = draw_gate_offset(jax.random.fold_in(key_of[13], 71), 0)
    head_gain = jnp.clip(1.0 + 0.18 * jax.random.normal(key_of[11], (HEADS * DV,), jnp.float32), 0.1, 1.9)
    w_out = noise(key_of[12], (HEADS * DV, D), (HEADS * DV) ** -0.5, 0.125, ((0, 2),))
    return {"tokens": tokens, "norm_gain": norm_gain, "w_query": w_query, "w_key": w_key, "w_value": w_value, "w_ogate": w_ogate, "w_igate": w_igate, "w_fgate": w_fgate, "conv_query": conv_query, "conv_key": conv_key, "gate_offset": gate_offset, "head_gain": head_gain, "w_out": w_out}


EPS = 1e-06
HIGHEST = lax.Precision.HIGHEST

def normalize_rows(values, gain_vec):
    widened = values.astype(jnp.float32)
    scaled = widened * lax.rsqrt(lax.optimization_barrier(jnp.mean(widened * widened, axis=-1, keepdims=True)) + EPS)
    return (scaled * gain_vec.astype(jnp.float32)).astype(jnp.bfloat16)

def causal_mix(values, weight):
    tap_count = weight.shape[0]
    seq_len = values.shape[0]
    leading = jnp.zeros((tap_count - 1, values.shape[1]), values.dtype)
    padded = jnp.concatenate([leading, values], axis=0).astype(jnp.float32)
    mixed_sum = jnp.zeros((seq_len, values.shape[1]), jnp.float32)
    for tap_index in range(tap_count):
        mixed_sum = mixed_sum + weight[tap_index].astype(jnp.float32) * padded[tap_index:tap_index + seq_len]
    return mixed_sum

def block_step(carried, inputs):
    states, norm_vec, levels = carried
    query_blk, key_blk, value_blk, gate_blk, forget_blk = inputs
    cumulative = jnp.cumsum(forget_blk, axis=0).T
    gate_rows = gate_blk.T
    span_len = cumulative.shape[1]
    causal = jnp.tril(jnp.ones((span_len, span_len), dtype=bool))
    log_weight = jnp.where(causal[None], cumulative[:, :, None] - cumulative[:, None, :] + gate_rows[:, None, :], -jnp.inf)
    carried_log = cumulative + levels[:, None]
    running_top = jnp.maximum(carried_log, lax.optimization_barrier(jnp.max(log_weight, axis=-1)))
    inner_weight = jnp.exp(log_weight - running_top[:, :, None])
    carried_scale = jnp.exp(carried_log - running_top)
    query_wide = query_blk.astype(jnp.float32)
    key_wide = key_blk.astype(jnp.float32)
    scores = jnp.einsum('thd,shd->hts', query_wide, key_wide, precision=HIGHEST) * inner_weight
    scores_low = lax.optimization_barrier(scores.astype(jnp.bfloat16)).astype(jnp.float32)
    numerator = carried_scale[:, :, None] * jnp.einsum('thd,hde->hte', query_wide, states, precision=HIGHEST)
    numerator = numerator + jnp.einsum('hts,she->hte', scores_low, value_blk.astype(jnp.float32), precision=HIGHEST)
    denominator = carried_scale * jnp.einsum('thd,hd->ht', query_wide, norm_vec, precision=HIGHEST) + lax.optimization_barrier(jnp.sum(scores, axis=-1))
    cell_out = numerator / jnp.maximum(jnp.abs(denominator), jnp.exp(-running_top))[:, :, None]
    last_log = cumulative[:, -1]
    write_log = last_log[:, None] - cumulative + gate_rows
    new_levels = jnp.maximum(last_log + levels, lax.optimization_barrier(jnp.max(write_log, axis=-1)))
    decay_scale = jnp.exp(last_log + levels - new_levels)
    write_weight = jnp.exp(write_log - new_levels[:, None])
    weighted = write_weight.T[:, :, None] * key_wide
    weighted_low = lax.optimization_barrier(weighted.astype(jnp.bfloat16)).astype(jnp.float32)
    new_states = decay_scale[:, None, None] * states + jnp.einsum('shd,she->hde', weighted_low, value_blk.astype(jnp.float32), precision=HIGHEST)
    new_norm = decay_scale[:, None] * norm_vec + lax.optimization_barrier(jnp.sum(weighted, axis=0))
    return ((new_states, new_norm, new_levels), jnp.transpose(cell_out, (1, 0, 2)))

def reference(tokens, norm_gain, w_query, w_key, w_value, w_ogate, w_igate, w_fgate, conv_query, conv_key, gate_offset, head_gain, w_out):
    normed = normalize_rows(tokens, norm_gain)
    query_pre = jnp.dot(normed, w_query, preferred_element_type=jnp.float32).astype(jnp.bfloat16)
    key_pre = jnp.dot(normed, w_key, preferred_element_type=jnp.float32).astype(jnp.bfloat16)
    value_pre = jnp.dot(normed, w_value, preferred_element_type=jnp.float32).astype(jnp.bfloat16)
    ogate_pre = jnp.dot(normed, w_ogate, preferred_element_type=jnp.float32).astype(jnp.bfloat16)
    input_pre = jnp.dot(normed, w_igate, preferred_element_type=jnp.float32)
    forget_pre = jnp.dot(normed, w_fgate, preferred_element_type=jnp.float32)
    input_gate = input_pre + jnp.repeat(gate_offset[0], SPAN, axis=0)
    log_forget = jax.nn.log_sigmoid(forget_pre + jnp.repeat(gate_offset[1], SPAN, axis=0))
    query_rows = jax.nn.silu(causal_mix(query_pre, conv_query)).astype(jnp.bfloat16).reshape(TOKENS, HEADS, DQK)
    key_rows = (jax.nn.silu(causal_mix(key_pre, conv_key)) * DQK ** (-0.5)).astype(jnp.bfloat16).reshape(TOKENS, HEADS, DQK)
    value_rows = value_pre.reshape(TOKENS, HEADS, DV)
    blocks = TOKENS // SPAN
    blocked = (query_rows.reshape(blocks, SPAN, HEADS, DQK), key_rows.reshape(blocks, SPAN, HEADS, DQK), value_rows.reshape(blocks, SPAN, HEADS, DV), input_gate.reshape(blocks, SPAN, HEADS), log_forget.reshape(blocks, SPAN, HEADS))
    initial = (jnp.zeros((HEADS, DQK, DV), jnp.float32), jnp.zeros((HEADS, DQK), jnp.float32), jnp.zeros((HEADS,), jnp.float32))
    _, cell_blocks = lax.scan(block_step, initial, blocked)
    cell_out = cell_blocks.reshape(TOKENS, HEADS, DV)
    cell_out = cell_out * lax.rsqrt(lax.optimization_barrier(jnp.mean(cell_out * cell_out, axis=-1, keepdims=True)) + EPS)
    hidden = cell_out.reshape(TOKENS, HEADS * DV) * head_gain.astype(jnp.float32) * jax.nn.sigmoid(ogate_pre.astype(jnp.float32))
    hidden = hidden.astype(jnp.bfloat16)
    return jnp.dot(hidden, w_out, preferred_element_type=jnp.float32).astype(jnp.bfloat16)
```

```python
import functools

import jax
import jax.numpy as jnp
from jax import lax
from jax.experimental import pallas as pl
from jax.experimental.pallas import tpu as pltpu
from jax.sharding import PartitionSpec as P

SPAN = 128
HALO = 16
EPS = 1e-06
EMPTY_LEVEL = -1e30
HIGHEST = lax.Precision.HIGHEST
MESH = pl.DeviceIdType.MESH
F32, BF16 = jnp.float32, jnp.bfloat16


def normalize(values, gain):
    widened = values.astype(F32)
    scaled = widened * lax.rsqrt(jnp.mean(widened * widened, axis=-1, keepdims=True) + EPS)
    return (scaled * gain).astype(BF16)


def dot_t(a, b):
    return lax.dot_general(a, b, (((1,), (1,)), ((), ())), preferred_element_type=F32)


def dot_tl(a, b):
    return lax.dot_general(a, b, (((0,), (0,)), ((), ())), preferred_element_type=F32)


def kernel(
    sp,
    tp,
    tokens_hbm,
    gain_ref,
    wq_hbm,
    wk_hbm,
    wv_hbm,
    wo_hbm,
    wi_ref,
    wf_ref,
    cq_ref,
    ck_ref,
    offset_ref,
    hgain_ref,
    wout_hbm,
    out_ref,
    ext,
    normed,
    wq,
    wk,
    wv,
    wo,
    wout,
    pre,
    key,
    query,
    value,
    ogate,
    numer,
    cols,
    hidden,
    sbuf,
    rbuf,
    meta,
    mbuf,
    pbuf,
    gbuf,
    sharesend,
    sharerecv,
    w_sem,
    t_sem,
    tsend_sem,
    trecv_sem,
    hsend_sem,
    hrecv_sem,
    psend_sem,
    precv_sem,
    msend_sem,
    mrecv_sem,
    gsend_sem,
    grecv_sem,
    osend_sem,
    orecv_sem,
):
    me = lax.axis_index("sp")
    core = lax.axis_index("tp")
    rows, model = tokens_hbm.shape
    seq_len = rows * tp
    blocks = seq_len // SPAN
    heads = offset_ref.shape[2]
    dqk = wq.shape[1] // heads
    dv = wv.shape[1] // heads
    piece_rows = sbuf.shape[1]
    head_first = core * heads

    own_rows = pl.ds(pl.multiple_of(HALO + core * rows, 16), rows)
    own_copy = pltpu.make_async_copy(tokens_hbm, ext.at[own_rows], t_sem)
    own_copy.start()
    streams = {}
    at = 0
    for name, hbm, vm in (
        ("v", wv_hbm, wv),
        ("k", wk_hbm, wk),
        ("q", wq_hbm, wq),
        ("o", wo_hbm, wo),
        ("out", wout_hbm, wout),
    ):
        streams[name] = []
        for c in range(0, hbm.shape[1], 512):
            cp = pltpu.make_async_copy(
                hbm.at[:, pl.ds(c, 512)], vm.at[:, pl.ds(c, 512)], w_sem.at[at]
            )
            cp.start()
            streams[name].append(cp)
            at += 1

    barrier = pltpu.get_barrier_semaphore()

    def greet(d, c):
        pl.semaphore_signal(
            barrier, inc=1, device_id=(lax.rem(me + d, sp), core), device_id_type=MESH
        )
        return c

    lax.fori_loop(1, sp, greet, 0)
    for d in range(1, tp):
        pl.semaphore_signal(
            barrier, inc=1, device_id=(me, lax.rem(core + d, tp)), device_id_type=MESH
        )
    pl.semaphore_wait(barrier, sp - 1 + tp - 1)

    token_sends = []
    for d in range(1, tp):
        cp = pltpu.make_async_remote_copy(
            src_ref=tokens_hbm,
            dst_ref=ext.at[own_rows],
            send_sem=tsend_sem.at[d],
            recv_sem=trecv_sem.at[d],
            device_id=(me, lax.rem(core + d, tp)),
            device_id_type=MESH,
        )
        cp.start()
        token_sends.append(cp)

    own_copy.wait()
    gain = gain_ref[...]
    normed[own_rows, :] = normalize(ext[own_rows, :], gain)
    for d in range(1, tp):
        token_sends[d - 1].wait_send()
        src_core = lax.rem(core + tp - d, tp)
        their = pl.ds(pl.multiple_of(HALO + src_core * rows, 16), rows)
        pltpu.make_async_remote_copy(
            src_ref=tokens_hbm,
            dst_ref=ext.at[their],
            send_sem=tsend_sem.at[d],
            recv_sem=trecv_sem.at[d],
            device_id=(me, src_core),
            device_id_type=MESH,
        ).wait_recv()
    halo = pltpu.make_async_remote_copy(
        src_ref=ext.at[pl.ds(seq_len, HALO)],
        dst_ref=ext.at[pl.ds(0, HALO)],
        send_sem=hsend_sem,
        recv_sem=hrecv_sem,
        device_id=(lax.rem(me + 1, sp), core),
        device_id_type=MESH,
    )

    @pl.when(me < sp - 1)
    def _():
        halo.start()

    for d in range(1, tp):
        src_core = lax.rem(core + tp - d, tp)
        their = pl.ds(pl.multiple_of(HALO + src_core * rows, 16), rows)
        normed[their, :] = normalize(ext[their, :], gain)

    body_rows = pl.ds(HALO, seq_len)

    gates_all = dot_t(
        jnp.concatenate([wi_ref[...], wf_ref[...]], axis=0), normed[body_rows, :]
    )
    total_heads = wi_ref.shape[0]
    in_rows = gates_all[:heads]
    fo_rows = gates_all[total_heads : total_heads + heads]
    for c in range(1, tp):
        in_rows = jnp.where(core == c, gates_all[c * heads : (c + 1) * heads], in_rows)
        fo_rows = jnp.where(
            core == c,
            gates_all[total_heads + c * heads : total_heads + (c + 1) * heads],
            fo_rows,
        )
    head_id = lax.broadcasted_iota(jnp.int32, (heads, SPAN), 0)

    def offsets(kind, b):
        spread = jnp.zeros((heads, SPAN), F32)
        for h in range(heads):
            spread = jnp.where(head_id == h, offset_ref[kind, b, h], spread)
        return spread

    upper = (
        lax.broadcasted_iota(jnp.int32, (SPAN, SPAN), 0)
        <= lax.broadcasted_iota(jnp.int32, (SPAN, SPAN), 1)
    ).astype(F32)
    gate, cum, tot = [], [], []
    for b in range(blocks):
        part = slice(b * SPAN, (b + 1) * SPAN)
        gate.append(in_rows[:, part] + offsets(0, b))
        x = fo_rows[:, part] + offsets(1, b)
        lf = jnp.minimum(x, 0.0) - jnp.log1p(jnp.exp(-jnp.abs(x)))
        lf8 = jnp.concatenate([lf, jnp.zeros((8 - heads, SPAN), F32)], axis=0) if heads < 8 else lf
        c = jnp.dot(lf8, upper, precision=HIGHEST, preferred_element_type=F32)[:heads]
        cum.append(c)
        tot.append(c[:, SPAN - 1 :])
    base = [jnp.zeros((heads, 1), F32)]
    for b in range(blocks):
        base.append(base[-1] + tot[b])
    tail = [None] * blocks
    acc = jnp.zeros((heads, 1), F32)
    for b in reversed(range(blocks)):
        tail[b] = acc
        acc = acc + tot[b]
    wlog = [tail[b] + (tot[b] - cum[b]) + gate[b] for b in range(blocks)]
    level = jnp.max(wlog[0], axis=1, keepdims=True)
    for b in range(1, blocks):
        level = jnp.maximum(level, jnp.max(wlog[b], axis=1, keepdims=True))
    wrows = [jnp.exp(w - level) for w in wlog]
    stacked = [jnp.concatenate([cum[b], wrows[b]], axis=0).T for b in range(blocks)]

    for c, cp in enumerate(streams["v"]):
        cp.wait()
        for n in range(c * 512, c * 512 + 512, 256):
            value[:, n : n + 256] = jnp.dot(
                normed[body_rows, :], wv[:, n : n + 256], preferred_element_type=F32
            ).astype(BF16)

    @pl.when(me < sp - 1)
    def _():
        halo.wait_send()

    @pl.when(me > 0)
    def _():
        halo.wait_recv()

    @pl.when(me == 0)
    def _():
        ext[pl.ds(0, HALO), :] = jnp.zeros((HALO, model), BF16)

    normed[pl.ds(0, HALO), :] = normalize(ext[pl.ds(0, HALO), :], gain)

    def project_mix(stream, w, taps_ref, dest, scale):
        for cp in stream:
            cp.wait()
        width = w.shape[1]
        for n in range(0, width, 256):
            pre[:, n : n + 256] = (
                jnp.dot(normed[...], w[:, n : n + 256], preferred_element_type=F32)
                .astype(BF16)
                .astype(F32)
            )
        taps = taps_ref[:, pl.ds(pl.multiple_of(core * width, 128), width)].astype(F32)
        count = taps.shape[0]
        for n in range(0, width, 128):
            mixed = jnp.zeros((seq_len, 128), F32)
            for j in range(count):
                mixed = (
                    mixed
                    + taps[j : j + 1, n : n + 128]
                    * pre[pl.ds(HALO - count + 1 + j, seq_len), n : n + 128]
                )
            dest[:, n : n + 128] = (mixed * jax.nn.sigmoid(mixed) * scale).astype(BF16)

    project_mix(streams["k"], wk, ck_ref, key, dqk**-0.5)

    for h in range(heads):
        weighted = [
            stacked[b][:, heads + h : heads + h + 1]
            * key[b * SPAN : (b + 1) * SPAN, h * dqk : (h + 1) * dqk].astype(F32)
            for b in range(blocks)
        ]
        norm = jnp.sum(weighted[0], axis=0, keepdims=True)
        for b in range(1, blocks):
            norm = norm + jnp.sum(weighted[b], axis=0, keepdims=True)
        state = dot_tl(
            jnp.concatenate([w.astype(BF16) for w in weighted], axis=0),
            value[:, h * dv : (h + 1) * dv],
        )
        per = dqk // piece_rows
        for p in range(per):
            sbuf[h * per + p] = state[p * piece_rows : (p + 1) * piece_rows].astype(BF16)
        meta[0, h : h + 1, :] = norm
    meta[1] = jnp.broadcast_to(base[blocks], (heads, dqk))
    meta[2] = jnp.broadcast_to(level, (heads, dqk))

    def piece_copy(source, target, d):
        return pltpu.make_async_remote_copy(
            src_ref=sbuf.at[target],
            dst_ref=rbuf.at[source],
            send_sem=psend_sem.at[d],
            recv_sem=precv_sem.at[source],
            device_id=(target, core),
            device_id_type=MESH,
        )

    def meta_copy(source, target, d):
        return pltpu.make_async_remote_copy(
            src_ref=meta,
            dst_ref=mbuf.at[source],
            send_sem=msend_sem.at[d],
            recv_sem=mrecv_sem.at[source],
            device_id=(target, core),
            device_id_type=MESH,
        )

    def prefix_copy(source, target):
        return pltpu.make_async_remote_copy(
            src_ref=pbuf.at[target],
            dst_ref=gbuf.at[source],
            send_sem=gsend_sem.at[target],
            recv_sem=grecv_sem.at[source],
            device_id=(target, core),
            device_id_type=MESH,
        )

    def send_one(d, c):
        target = lax.rem(me + d, sp)
        meta_copy(me, target, d).start()
        piece_copy(me, target, d).start()
        return c

    lax.fori_loop(1, sp, send_one, 0)
    rbuf[me] = sbuf[me]
    mbuf[me] = meta[...]

    project_mix(streams["q"], wq, cq_ref, query, 1.0)

    causal = lax.broadcasted_iota(jnp.int32, (SPAN, SPAN), 0) >= lax.broadcasted_iota(
        jnp.int32, (SPAN, SPAN), 1
    )

    def intra(h):
        for i in range(blocks):
            col = stacked[i][:, h : h + 1]
            logs = []
            top = None
            for j in range(i + 1):
                row = (gate[j][h : h + 1] - cum[j][h : h + 1]) + (
                    base[i][h : h + 1] - base[j][h : h + 1]
                )
                tile = col + row
                if j == i:
                    tile = jnp.where(causal, tile, -jnp.inf)
                logs.append(tile)
                t = jnp.max(tile, axis=1, keepdims=True)
                top = t if top is None else jnp.maximum(top, t)
            q = query[i * SPAN : (i + 1) * SPAN, h * dqk : (h + 1) * dqk]
            den = jnp.zeros((SPAN, 1), F32)
            num = jnp.zeros((SPAN, dv), F32)
            for j in range(i + 1):
                k = key[j * SPAN : (j + 1) * SPAN, h * dqk : (h + 1) * dqk]
                scores = dot_t(q, k) * jnp.exp(logs[j] - top)
                den = den + jnp.sum(scores, axis=1, keepdims=True)
                num = num + jnp.dot(
                    scores.astype(BF16),
                    value[j * SPAN : (j + 1) * SPAN, h * dv : (h + 1) * dv],
                    preferred_element_type=F32,
                )
            numer[i * SPAN : (i + 1) * SPAN, h * dv : (h + 1) * dv] = num
            cols[h, i * SPAN : (i + 1) * SPAN, 0:1] = den
            cols[h, i * SPAN : (i + 1) * SPAN, 1:2] = top

    for h in range(heads):
        intra(h)

    per_head = sp // heads
    my_head = me // per_head
    small_id = lax.broadcasted_iota(jnp.int32, (heads, dqk), 0)

    def pick(x):
        r = jnp.sum(jnp.where(small_id == my_head, x, 0.0), axis=0, keepdims=True)
        return jnp.concatenate([r] * (dv // dqk), axis=1)

    def combine(i, carry):
        lev, nor, piece, lev_in, nor_in = carry
        j = i - 1

        @pl.when(j != me)
        def _():
            meta_copy(j, me, 0).wait_recv()
            piece_copy(j, me, 0).wait_recv()

        shifted = lev + mbuf[j, 1]
        new_lev = jnp.maximum(shifted, mbuf[j, 2])
        one, two = jnp.exp(shifted - new_lev), jnp.exp(mbuf[j, 2] - new_lev)
        nor = one * nor + two * mbuf[j, 0]
        piece = pick(one) * piece + pick(two) * rbuf[j].astype(F32)
        pbuf[i] = piece.astype(BF16)

        @pl.when(i == me)
        def _():
            gbuf[me] = piece.astype(BF16)

        @pl.when(jnp.logical_and(i > 1, j != me))
        def _():
            prefix_copy(me, j).start()

        lev_in = jnp.where(i == me, new_lev, lev_in)
        nor_in = jnp.where(i == me, nor, nor_in)
        return new_lev, nor, piece, lev_in, nor_in

    empty = jnp.full((heads, dqk), EMPTY_LEVEL, F32)
    none = jnp.zeros((heads, dqk), F32)
    _, _, _, lev_in, nor_in = lax.fori_loop(
        1, sp, combine, (empty, none, jnp.zeros((piece_rows, dv), F32), empty, none)
    )

    @pl.when(me != sp - 1)
    def _():
        prefix_copy(me, sp - 1).start()

    @pl.when(me != sp - 1)
    def _():
        meta_copy(sp - 1, me, 0).wait_recv()
        piece_copy(sp - 1, me, 0).wait_recv()

    for c, cp in enumerate(streams["o"]):
        cp.wait()
        for n in range(c * 512, c * 512 + 512, 256):
            ogate[:, n : n + 256] = jnp.dot(
                normed[body_rows, :], wo[:, n : n + 256], preferred_element_type=F32
            ).astype(BF16)

    @pl.when(me == 0)
    def _():
        gbuf[...] = jnp.zeros(gbuf.shape, BF16)

    def take(d, c):
        prefix_copy(lax.rem(me + d, sp), me).wait_recv()
        return c

    @pl.when(me > 0)
    def _():
        lax.fori_loop(1, sp, take, 0)

    per = dqk // piece_rows
    for h in range(heads):
        state = jnp.concatenate([gbuf[h * per + p] for p in range(per)], axis=0)
        hgain = hgain_ref[:, pl.ds(pl.multiple_of((head_first + h) * dv, 128), dv)]
        for i in range(blocks):
            part = slice(i * SPAN, (i + 1) * SPAN)
            q = query[part, h * dqk : (h + 1) * dqk]
            carried = (stacked[i][:, h : h + 1] + base[i][h : h + 1]) + lev_in[h : h + 1, 0:1]
            den, own_top = cols[h, part, 0:1], cols[h, part, 1:2]
            top = jnp.maximum(own_top, carried)
            own, old = jnp.exp(own_top - top), jnp.exp(carried - top)
            from_norm = jnp.sum(q.astype(F32) * nor_in[h : h + 1], axis=1, keepdims=True)
            den = own * den + old * from_norm
            num = own * numer[part, h * dv : (h + 1) * dv] + old * jnp.dot(
                q, state, preferred_element_type=F32
            )
            cell = num / jnp.maximum(jnp.abs(den), jnp.exp(-top))
            cell = cell * lax.rsqrt(jnp.mean(cell * cell, axis=-1, keepdims=True) + EPS)
            hidden[part, h * dv : (h + 1) * dv] = (
                cell * hgain * jax.nn.sigmoid(ogate[part, h * dv : (h + 1) * dv].astype(F32))
            ).astype(BF16)

    sends = []
    chunks = len(streams["out"])
    for c, cp in enumerate(streams["out"]):
        cp.wait()
    for d in range(1, tp):
        target = lax.rem(core + d, tp)
        theirs = pl.ds(pl.multiple_of(target * rows, 16), rows)
        for c in range(chunks):
            sharesend[d - 1, c] = jnp.dot(
                hidden[theirs, :], wout[:, c * 512 : (c + 1) * 512], preferred_element_type=F32
            ).astype(BF16)
            cp = pltpu.make_async_remote_copy(
                src_ref=sharesend.at[d - 1, c],
                dst_ref=sharerecv.at[d - 1, c],
                send_sem=osend_sem.at[d - 1, c],
                recv_sem=orecv_sem.at[d - 1, c],
                device_id=(me, target),
                device_id_type=MESH,
            )
            cp.start()
            sends.append(cp)
    mine = pl.ds(pl.multiple_of(core * rows, 16), rows)
    for c in range(chunks):
        total = jnp.dot(
            hidden[mine, :], wout[:, c * 512 : (c + 1) * 512], preferred_element_type=F32
        )
        for d in range(1, tp):
            sends[(d - 1) * chunks + c].wait_recv()
            total = total + sharerecv[d - 1, c].astype(F32)
        out_ref[:, c * 512 : (c + 1) * 512] = total.astype(BF16)

    for cp in sends:
        cp.wait_send()

    def settle(d, c):
        target = lax.rem(me + d, sp)
        meta_copy(me, target, d).wait_send()
        piece_copy(me, target, d).wait_send()

        @pl.when(target > 0)
        def _():
            prefix_copy(me, target).wait_send()

        return c

    lax.fori_loop(1, sp, settle, 0)


def body(sp, tp, tokens, norm_gain, wq, wk, wv, wo, wi, wf, cq, ck, offset, hgain, wout):
    rows, model = tokens.shape
    seq_len = rows * tp
    heads = offset.shape[2]
    qk, vd = wq.shape[1], wv.shape[1]
    dqk, dv = qk // heads, vd // heads
    piece = qk // sp
    chunks = wout.shape[1] // 512
    streams = (2 * qk + 2 * vd + wout.shape[1]) // 512
    hbm = pl.BlockSpec(memory_space=pl.ANY)
    vmem = pl.BlockSpec(memory_space=pltpu.VMEM)
    smem = pl.BlockSpec(memory_space=pltpu.SMEM)
    dma = pltpu.SemaphoreType.DMA
    return pl.pallas_call(
        functools.partial(kernel, sp, tp),
        out_shape=jax.ShapeDtypeStruct((rows, wout.shape[1]), BF16),
        in_specs=[hbm, vmem, hbm, hbm, hbm, hbm, vmem, vmem, vmem, vmem, smem, vmem, hbm],
        out_specs=vmem,
        scratch_shapes=[
            pltpu.VMEM((HALO + seq_len, model), BF16),
            pltpu.VMEM((HALO + seq_len, model), BF16),
            pltpu.VMEM(wq.shape, BF16),
            pltpu.VMEM(wk.shape, BF16),
            pltpu.VMEM(wv.shape, BF16),
            pltpu.VMEM(wo.shape, BF16),
            pltpu.VMEM(wout.shape, BF16),
            pltpu.VMEM((HALO + seq_len, qk), F32),
            pltpu.VMEM((seq_len, qk), BF16),
            pltpu.VMEM((seq_len, qk), BF16),
            pltpu.VMEM((seq_len, vd), BF16),
            pltpu.VMEM((seq_len, vd), BF16),
            pltpu.VMEM((seq_len, vd), F32),
            pltpu.VMEM((heads, seq_len, 128), F32),
            pltpu.VMEM((seq_len, vd), BF16),
            pltpu.VMEM((sp, piece, dv), BF16),
            pltpu.VMEM((sp, piece, dv), BF16),
            pltpu.VMEM((3, heads, dqk), F32),
            pltpu.VMEM((sp, 3, heads, dqk), F32),
            pltpu.VMEM((sp, piece, dv), BF16),
            pltpu.VMEM((sp, piece, dv), BF16),
            pltpu.VMEM((tp - 1, chunks, rows, 512), BF16),
            pltpu.VMEM((tp - 1, chunks, rows, 512), BF16),
            dma((streams,)),
            dma,
            dma((tp,)),
            dma((tp,)),
            dma,
            dma,
            dma((sp,)),
            dma((sp,)),
            dma((sp,)),
            dma((sp,)),
            dma((sp,)),
            dma((sp,)),
            dma((tp - 1, chunks)),
            dma((tp - 1, chunks)),
        ],
        compiler_params=pltpu.CompilerParams(
            collective_id=0, has_side_effects=True, vmem_limit_bytes=60 * 1024 * 1024
        ),
    )(
        tokens,
        norm_gain.reshape(1, model),
        wq,
        wk,
        wv,
        wo,
        wi.T,
        wf.T,
        cq,
        ck,
        offset,
        hgain.reshape(1, hgain.shape[0]),
        wout,
    )


def solution(mesh):
    in_specs = (
        P(("sp", "tp"), None),
        P(),
        P(None, "tp"),
        P(None, "tp"),
        P(None, "tp"),
        P(None, "tp"),
        P(),
        P(),
        P(),
        P(),
        P(None, "sp", "tp"),
        P(),
        P("tp", None),
    )
    out_specs = P(("sp", "tp"), None)
    step = functools.partial(body, mesh.shape["sp"], mesh.shape["tp"])
    return jax.shard_map(step, mesh=mesh, in_specs=in_specs, out_specs=out_specs, check_vma=False)
```

```python
import functools

import jax
import jax.numpy as jnp
from jax import lax
from jax.experimental import pallas as pl
from jax.experimental.pallas import tpu as pltpu
from jax.sharding import PartitionSpec as P

SPAN = 128
HALO = 16
EPS = 1e-06
EMPTY_LEVEL = -1e30
HIGHEST = lax.Precision.HIGHEST
MESH = pl.DeviceIdType.MESH
F32, BF16 = jnp.float32, jnp.bfloat16


def normalize(values, gain):
    widened = values.astype(F32)
    scaled = widened * lax.rsqrt(jnp.mean(widened * widened, axis=-1, keepdims=True) + EPS)
    return (scaled * gain).astype(BF16)


def dot_t(a, b):
    return lax.dot_general(a, b, (((1,), (1,)), ((), ())), preferred_element_type=F32)


def dot_tl(a, b):
    return lax.dot_general(a, b, (((0,), (0,)), ((), ())), preferred_element_type=F32)


def kernel(
    sp,
    tp,
    tokens_hbm,
    gain_hbm,
    wq_hbm,
    wk_hbm,
    wv_hbm,
    wo_hbm,
    wi_hbm,
    wf_hbm,
    cq_hbm,
    ck_hbm,
    offset_hbm,
    hgain_hbm,
    wout_hbm,
    out_ref,
    gain_ref,
    wi_ref,
    wf_ref,
    cq_ref,
    ck_ref,
    offset_ref,
    hgain_ref,
    ext_own,
    ext_oth,
    nor_own,
    nor_oth,
    wq,
    wk,
    wv,
    wo,
    wout,
    gcol,
    kpre,
    qpre,
    key,
    query,
    value,
    ogate,
    numer,
    cols,
    hidden,
    sbuf,
    rbuf,
    meta,
    mbuf,
    nmeta,
    nbuf,
    scales,
    pbuf,
    gbuf,
    sharesend,
    sharerecv,
    w_sem,
    t_sem,
    s_sem,
    tsend_sem,
    trecv_sem,
    hsend_sem,
    hrecv_sem,
    psend_sem,
    precv_sem,
    msend_sem,
    mrecv_sem,
    nsend_sem,
    nrecv_sem,
    gsend_sem,
    grecv_sem,
    osend_sem,
    orecv_sem,
):
    me = lax.axis_index("sp")
    core = lax.axis_index("tp")
    rows, model = tokens_hbm.shape
    seq_len = rows * tp
    blocks = seq_len // SPAN
    heads = offset_hbm.shape[2]
    dqk = wq.shape[1] // heads
    dv = wv.shape[1] // heads
    piece_rows = sbuf.shape[1]
    head_first = core * heads
    last = tp - 1

    barrier = pltpu.get_barrier_semaphore()

    def signal(to_sp, to_tp):
        pl.semaphore_signal(barrier, inc=1, device_id=(to_sp, to_tp), device_id_type=MESH)

    def greet(d, c):
        signal(lax.rem(me + d, sp), core)
        return c

    lax.fori_loop(1, sp, greet, 0)
    for d in range(1, tp):
        signal(me, lax.rem(core + d, tp))

    @pl.when(core == last)
    def _():
        for c in range(tp - 1):
            signal(lax.rem(me + 1, sp), c)

    @pl.when(core != last)
    def _():
        signal(lax.rem(me + sp - 1, sp), last)

    own_copy = pltpu.make_async_copy(tokens_hbm, ext_own, t_sem)
    own_copy.start()
    small = []
    for n, (src, dst) in enumerate(
        (
            (gain_hbm, gain_ref),
            (wi_hbm, wi_ref),
            (wf_hbm, wf_ref),
            (ck_hbm, ck_ref),
            (cq_hbm, cq_ref),
            (offset_hbm, offset_ref),
            (hgain_hbm, hgain_ref),
        )
    ):
        cp = pltpu.make_async_copy(src, dst, s_sem.at[n])
        cp.start()
        small.append(cp)
    streams = {}
    at = 0
    for name, hbm, vm in (
        ("v", wv_hbm, wv),
        ("k", wk_hbm, wk),
        ("q", wq_hbm, wq),
        ("o", wo_hbm, wo),
        ("out", wout_hbm, wout),
    ):
        streams[name] = []
        for c in range(0, hbm.shape[1], 512):
            cp = pltpu.make_async_copy(
                hbm.at[:, pl.ds(c, 512)], vm.at[:, pl.ds(c, 512)], w_sem.at[at]
            )
            cp.start()
            streams[name].append(cp)
            at += 1

    for cp in small:
        cp.wait()
    own_copy.wait()
    gain = gain_ref[...]
    nor_own[...] = normalize(ext_own[...], gain)
    own = pl.ds(pl.multiple_of(core * rows, 16), rows)
    gate_weights = jnp.concatenate(
        [
            wi_ref[...].astype(F32),
            wf_ref[...].astype(F32),
            jnp.zeros((128 - 2 * wi_ref.shape[0], model), F32),
        ],
        axis=0,
    ).astype(BF16)
    gcol[own, :] = dot_t(nor_own[...], gate_weights)

    pl.semaphore_wait(barrier, sp - 1 + tp - 1 + jnp.where(core == last, tp - 1, 1))

    def token_copy(d, target, source):
        return pltpu.make_async_remote_copy(
            src_ref=ext_own,
            dst_ref=ext_oth.at[d - 1, pl.ds(0, rows)],
            send_sem=tsend_sem.at[d - 1],
            recv_sem=trecv_sem.at[d - 1],
            device_id=(me, target),
            device_id_type=MESH,
        )

    def halo_copy(c):
        return pltpu.make_async_remote_copy(
            src_ref=ext_own.at[pl.ds(rows - HALO, HALO)],
            dst_ref=ext_oth.at[tp - 2, pl.ds(rows, HALO)],
            send_sem=hsend_sem.at[c],
            recv_sem=hrecv_sem,
            device_id=(lax.rem(me + 1, sp), c),
            device_id_type=MESH,
        )

    sends_halo = jnp.logical_and(core == last, me < sp - 1)

    @pl.when(sends_halo)
    def _():
        for c in range(tp):
            halo_copy(c).start()

    for d in range(1, tp):
        token_copy(d, lax.rem(core + d, tp), None).start()

    def project(w, lhs, n):
        return jnp.dot(lhs, w[:, n : n + 256], preferred_element_type=F32).astype(BF16)

    qk, vd = wq.shape[1], wv.shape[1]
    pre_own = pl.ds(pl.multiple_of(HALO + core * rows, 16), rows)

    for c, cp in enumerate(streams["v"]):
        cp.wait()
        for n in range(c * 512, c * 512 + 512, 256):
            value[own, n : n + 256] = project(wv, nor_own[...], n)
    for cp in streams["k"]:
        cp.wait()
    for n in range(0, qk, 256):
        kpre[pre_own, n : n + 256] = project(wk, nor_own[...], n).astype(F32)

    @pl.when(sends_halo)
    def _():
        for c in range(tp):
            halo_copy(c).wait_send()

    for d in range(1, tp):
        cp = token_copy(d, lax.rem(core + d, tp), None)
        cp.wait_send()
        cp.wait_recv()
    for d in range(1, tp):
        nor_oth[d - 1, pl.ds(0, rows), :] = normalize(ext_oth[d - 1, pl.ds(0, rows), :], gain)

    def place(d):
        return lax.rem(core + tp - d, tp) * rows

    for d in range(1, tp):
        gcol[pl.ds(pl.multiple_of(place(d), 16), rows), :] = dot_t(
            nor_oth[d - 1, pl.ds(0, rows), :], gate_weights
        )

    gates_all = jnp.concatenate(
        [gcol[b * SPAN : (b + 1) * SPAN, :].T for b in range(blocks)], axis=1
    )
    total_heads = wi_ref.shape[0]
    in_rows = gates_all[:heads]
    fo_rows = gates_all[total_heads : total_heads + heads]
    for c in range(1, tp):
        in_rows = jnp.where(core == c, gates_all[c * heads : (c + 1) * heads], in_rows)
        fo_rows = jnp.where(
            core == c,
            gates_all[total_heads + c * heads : total_heads + (c + 1) * heads],
            fo_rows,
        )
    head_id = lax.broadcasted_iota(jnp.int32, (heads, SPAN), 0)

    def offsets(kind, b):
        spread = jnp.zeros((heads, SPAN), F32)
        for h in range(heads):
            spread = jnp.where(head_id == h, offset_ref[kind, b : b + 1, h : h + 1], spread)
        return spread

    upper = (
        lax.broadcasted_iota(jnp.int32, (SPAN, SPAN), 0)
        <= lax.broadcasted_iota(jnp.int32, (SPAN, SPAN), 1)
    ).astype(F32)
    gate, cum, tot = [], [], []
    for b in range(blocks):
        part = slice(b * SPAN, (b + 1) * SPAN)
        gate.append(in_rows[:, part] + offsets(0, b))
        x = fo_rows[:, part] + offsets(1, b)
        lf = jnp.minimum(x, 0.0) - jnp.log1p(jnp.exp(-jnp.abs(x)))
        lf8 = jnp.concatenate([lf, jnp.zeros((8 - heads, SPAN), F32)], axis=0) if heads < 8 else lf
        c = jnp.dot(lf8, upper, precision=HIGHEST, preferred_element_type=F32)[:heads]
        cum.append(c)
        tot.append(c[:, SPAN - 1 :])
    base = [jnp.zeros((heads, 1), F32)]
    for b in range(blocks):
        base.append(base[-1] + tot[b])
    tail = [None] * blocks
    acc = jnp.zeros((heads, 1), F32)
    for b in reversed(range(blocks)):
        tail[b] = acc
        acc = acc + tot[b]
    wlog = [tail[b] + (tot[b] - cum[b]) + gate[b] for b in range(blocks)]
    level = jnp.max(wlog[0], axis=1, keepdims=True)
    for b in range(1, blocks):
        level = jnp.maximum(level, jnp.max(wlog[b], axis=1, keepdims=True))
    wrows = [jnp.exp(w - level) for w in wlog]
    stacked = [jnp.concatenate([cum[b], wrows[b]], axis=0).T for b in range(blocks)]

    def to_peer(src, dst, ssem, rsem, target):
        return pltpu.make_async_remote_copy(
            src_ref=src,
            dst_ref=dst,
            send_sem=ssem,
            recv_sem=rsem,
            device_id=(target, core),
            device_id_type=MESH,
        )

    def meta_copy(source, target):
        return to_peer(meta, mbuf.at[source], msend_sem.at[target], mrecv_sem.at[source], target)

    def norm_copy(source, target):
        return to_peer(nmeta, nbuf.at[source], nsend_sem.at[target], nrecv_sem.at[source], target)

    def piece_copy(source, target):
        return to_peer(
            sbuf.at[target], rbuf.at[source], psend_sem.at[target], precv_sem.at[source], target
        )

    def prefix_copy(source, target):
        return to_peer(
            pbuf.at[target], gbuf.at[source], gsend_sem.at[target], grecv_sem.at[source], target
        )

    meta[0] = jnp.broadcast_to(base[blocks], (heads, dqk))
    meta[1] = jnp.broadcast_to(level, (heads, dqk))

    for n in range(0, vd, 256):
        for d in range(1, tp):
            value[pl.ds(pl.multiple_of(place(d), 16), rows), n : n + 256] = project(
                wv, nor_oth[d - 1, pl.ds(0, rows), :], n
            )

    def send_meta(d, c):
        meta_copy(me, lax.rem(me + d, sp)).start()
        return c

    lax.fori_loop(1, sp, send_meta, 0)
    mbuf[me] = meta[...]

    @pl.when(me > 0)
    def _():
        halo_copy(core).wait_recv()

    @pl.when(me == 0)
    def _():
        ext_oth[tp - 2, pl.ds(rows, HALO), :] = jnp.zeros((HALO, model), BF16)

    nor_oth[tp - 2, pl.ds(rows, HALO), :] = normalize(ext_oth[tp - 2, pl.ds(rows, HALO), :], gain)

    def rest_of(pre, w, n):
        for d in range(1, tp):
            more = HALO if d == tp - 1 else 0
            got = project(w, nor_oth[d - 1, pl.ds(0, rows + more), :], n).astype(F32)
            pre[pl.ds(pl.multiple_of(HALO + place(d), 16), rows), n : n + 256] = got[:rows]
            if more:
                pre[pl.ds(0, HALO), n : n + 256] = got[rows:]

    def mix(pre, taps_ref, dest, scale, n):
        taps = taps_ref[:, pl.ds(pl.multiple_of(core * qk + n, 128), 128)].astype(F32)
        count = taps.shape[0]
        mixed = jnp.zeros((seq_len, 128), F32)
        for j in range(count):
            mixed = (
                mixed
                + taps[j : j + 1, :] * pre[pl.ds(HALO - count + 1 + j, seq_len), n : n + 128]
            )
        dest[:, n : n + 128] = (mixed * jax.nn.sigmoid(mixed) * scale).astype(BF16)

    per = sp // heads
    for h in range(heads):
        if (h * dqk) % 256 == 0:
            rest_of(kpre, wk, h * dqk)
        mix(kpre, ck_ref, key, dqk**-0.5, h * dqk)
        weighted = [
            stacked[b][:, heads + h : heads + h + 1]
            * key[b * SPAN : (b + 1) * SPAN, h * dqk : (h + 1) * dqk].astype(F32)
            for b in range(blocks)
        ]
        norm = jnp.sum(weighted[0], axis=0, keepdims=True)
        for b in range(1, blocks):
            norm = norm + jnp.sum(weighted[b], axis=0, keepdims=True)
        state = dot_tl(
            jnp.concatenate([w.astype(BF16) for w in weighted], axis=0),
            value[:, h * dv : (h + 1) * dv],
        )
        for p in range(per):
            sbuf[p * heads + h] = state[p * piece_rows : (p + 1) * piece_rows].astype(BF16)
        nmeta[h : h + 1, :] = norm
        for p in range(per):
            target = p * heads + h

            @pl.when(me != target)
            def _():
                piece_copy(me, target).start()

            @pl.when(me == target)
            def _():
                rbuf[target] = sbuf[target]

    def send_norm(d, c):
        norm_copy(me, lax.rem(me + d, sp)).start()
        return c

    lax.fori_loop(1, sp, send_norm, 0)
    nbuf[me] = nmeta[...]

    for cp in streams["q"]:
        cp.wait()
    for n in range(0, qk, 256):
        qpre[pre_own, n : n + 256] = project(wq, nor_own[...], n).astype(F32)
        rest_of(qpre, wq, n)
        for m in range(n, n + 256, 128):
            mix(qpre, cq_ref, query, 1.0, m)

    my_head = lax.rem(me, heads)
    small_id = lax.broadcasted_iota(jnp.int32, (heads, dqk), 0)

    def weigh(i, carry):
        lev, lev_in = carry
        j = i - 1

        @pl.when(j != me)
        def _():
            meta_copy(j, me).wait_recv()

        shifted = lev + mbuf[j, 0]
        new_lev = jnp.maximum(shifted, mbuf[j, 1])
        one, two = jnp.exp(shifted - new_lev), jnp.exp(mbuf[j, 1] - new_lev)
        scales[i, 0] = one
        scales[i, 1] = two
        return new_lev, jnp.where(i == me, new_lev, lev_in)

    empty = jnp.full((heads, dqk), EMPTY_LEVEL, F32)
    _, lev_in = lax.fori_loop(1, sp, weigh, (empty, empty))

    causal = lax.broadcasted_iota(jnp.int32, (SPAN, SPAN), 0) >= lax.broadcasted_iota(
        jnp.int32, (SPAN, SPAN), 1
    )

    def intra(h):
        for i in range(blocks):
            col = stacked[i][:, h : h + 1]
            logs = []
            top = None
            for j in range(i + 1):
                row = (gate[j][h : h + 1] - cum[j][h : h + 1]) + (
                    base[i][h : h + 1] - base[j][h : h + 1]
                )
                tile = col + row
                if j == i:
                    tile = jnp.where(causal, tile, -jnp.inf)
                logs.append(tile)
                t = jnp.max(tile, axis=1, keepdims=True)
                top = t if top is None else jnp.maximum(top, t)
            q = query[i * SPAN : (i + 1) * SPAN, h * dqk : (h + 1) * dqk]
            den = jnp.zeros((SPAN, 1), F32)
            num = jnp.zeros((SPAN, dv), F32)
            for j in range(i + 1):
                k = key[j * SPAN : (j + 1) * SPAN, h * dqk : (h + 1) * dqk]
                scores = dot_t(q, k) * jnp.exp(logs[j] - top)
                den = den + jnp.sum(scores, axis=1, keepdims=True)
                num = num + jnp.dot(
                    scores.astype(BF16),
                    value[j * SPAN : (j + 1) * SPAN, h * dv : (h + 1) * dv],
                    preferred_element_type=F32,
                )
            numer[i * SPAN : (i + 1) * SPAN, h * dv : (h + 1) * dv] = num
            cols[h, i * SPAN : (i + 1) * SPAN, 0:1] = den
            cols[h, i * SPAN : (i + 1) * SPAN, 1:2] = top

    for h in range(heads // 2):
        intra(h)

    def pick(x):
        r = jnp.sum(jnp.where(small_id == my_head, x, 0.0), axis=0, keepdims=True)
        return jnp.concatenate([r] * (dv // dqk), axis=1)

    def combine(i, piece):
        j = i - 1
        one, two = pick(scales[i, 0]), pick(scales[i, 1])

        @pl.when(j != me)
        def _():
            piece_copy(j, me).wait_recv()

        piece = one * piece + two * rbuf[j].astype(F32)
        pbuf[i] = piece.astype(BF16)

        @pl.when(i == me)
        def _():
            gbuf[me] = piece.astype(BF16)

        @pl.when(jnp.logical_and(i > 1, j != me))
        def _():
            prefix_copy(me, j).start()

        return piece

    lax.fori_loop(1, sp, combine, jnp.zeros((piece_rows, dv), F32))

    @pl.when(me != sp - 1)
    def _():
        prefix_copy(me, sp - 1).start()

    for h in range(heads // 2, heads):
        intra(h)

    for c, cp in enumerate(streams["o"]):
        cp.wait()
        for n in range(c * 512, c * 512 + 512, 256):
            ogate[own, n : n + 256] = project(wo, nor_own[...], n)
            for d in range(1, tp):
                ogate[pl.ds(pl.multiple_of(place(d), 16), rows), n : n + 256] = project(
                    wo, nor_oth[d - 1, pl.ds(0, rows), :], n
                )

    @pl.when(me != sp - 1)
    def _():
        meta_copy(sp - 1, me).wait_recv()
        piece_copy(sp - 1, me).wait_recv()

    def take_norm(d, c):
        norm_copy(lax.rem(me + d, sp), me).wait_recv()
        return c

    lax.fori_loop(1, sp, take_norm, 0)
    nor_in = lax.fori_loop(
        1,
        me + 1,
        lambda i, nor: scales[i, 0] * nor + scales[i, 1] * nbuf[i - 1],
        jnp.zeros((heads, dqk), F32),
    )

    @pl.when(me == 0)
    def _():
        gbuf[...] = jnp.zeros(gbuf.shape, BF16)

    for h in range(heads):
        for p in range(per):
            source = p * heads + h

            @pl.when(jnp.logical_and(me > 0, me != source))
            def _():
                prefix_copy(source, me).wait_recv()

        state = jnp.concatenate([gbuf[p * heads + h] for p in range(per)], axis=0)
        hgain = hgain_ref[:, pl.ds(pl.multiple_of((head_first + h) * dv, 128), dv)]
        for i in range(blocks):
            part = slice(i * SPAN, (i + 1) * SPAN)
            q = query[part, h * dqk : (h + 1) * dqk]
            carried = (stacked[i][:, h : h + 1] + base[i][h : h + 1]) + lev_in[h : h + 1, 0:1]
            den, own_top = cols[h, part, 0:1], cols[h, part, 1:2]
            top = jnp.maximum(own_top, carried)
            new, old = jnp.exp(own_top - top), jnp.exp(carried - top)
            from_norm = jnp.sum(q.astype(F32) * nor_in[h : h + 1], axis=1, keepdims=True)
            den = new * den + old * from_norm
            num = new * numer[part, h * dv : (h + 1) * dv] + old * jnp.dot(
                q, state, preferred_element_type=F32
            )
            cell = num / jnp.maximum(jnp.abs(den), jnp.exp(-top))
            cell = cell * lax.rsqrt(jnp.mean(cell * cell, axis=-1, keepdims=True) + EPS)
            hidden[part, h * dv : (h + 1) * dv] = (
                cell * hgain * jax.nn.sigmoid(ogate[part, h * dv : (h + 1) * dv].astype(F32))
            ).astype(BF16)

    sends = []
    chunks = len(streams["out"])
    for c, cp in enumerate(streams["out"]):
        cp.wait()
    for d in range(1, tp):
        target = lax.rem(core + d, tp)
        theirs = pl.ds(pl.multiple_of(target * rows, 16), rows)
        for c in range(chunks):
            sharesend[d - 1, c] = jnp.dot(
                hidden[theirs, :], wout[:, c * 512 : (c + 1) * 512], preferred_element_type=F32
            ).astype(BF16)
            cp = pltpu.make_async_remote_copy(
                src_ref=sharesend.at[d - 1, c],
                dst_ref=sharerecv.at[d - 1, c],
                send_sem=osend_sem.at[d - 1, c],
                recv_sem=orecv_sem.at[d - 1, c],
                device_id=(me, target),
                device_id_type=MESH,
            )
            cp.start()
            sends.append(cp)
    for c in range(chunks):
        total = jnp.dot(
            hidden[own, :], wout[:, c * 512 : (c + 1) * 512], preferred_element_type=F32
        )
        for d in range(1, tp):
            sends[(d - 1) * chunks + c].wait_recv()
            total = total + sharerecv[d - 1, c].astype(F32)
        out_ref[:, c * 512 : (c + 1) * 512] = total.astype(BF16)

    for cp in sends:
        cp.wait_send()

    def settle(d, c):
        target = lax.rem(me + d, sp)
        meta_copy(me, target).wait_send()
        norm_copy(me, target).wait_send()
        piece_copy(me, target).wait_send()

        @pl.when(target > 0)
        def _():
            prefix_copy(me, target).wait_send()

        return c

    lax.fori_loop(1, sp, settle, 0)


def body(sp, tp, tokens, norm_gain, wq, wk, wv, wo, wi, wf, cq, ck, offset, hgain, wout):
    rows, model = tokens.shape
    seq_len = rows * tp
    heads = offset.shape[2]
    qk, vd = wq.shape[1], wv.shape[1]
    dqk, dv = qk // heads, vd // heads
    piece = qk // sp
    chunks = wout.shape[1] // 512
    streams = (2 * qk + 2 * vd + wout.shape[1]) // 512
    hbm = pl.BlockSpec(memory_space=pl.ANY)
    vmem = pl.BlockSpec(memory_space=pltpu.VMEM)
    dma = pltpu.SemaphoreType.DMA
    return pl.pallas_call(
        functools.partial(kernel, sp, tp),
        out_shape=jax.ShapeDtypeStruct((rows, wout.shape[1]), BF16),
        in_specs=[hbm] * 13,
        out_specs=vmem,
        scratch_shapes=[
            pltpu.VMEM((1, model), F32),
            pltpu.VMEM((wi.shape[1], model), BF16),
            pltpu.VMEM((wf.shape[1], model), BF16),
            pltpu.VMEM(cq.shape, BF16),
            pltpu.VMEM(ck.shape, BF16),
            pltpu.VMEM(offset.shape, F32),
            pltpu.VMEM((1, hgain.shape[0]), F32),
            pltpu.VMEM((rows, model), BF16),
            pltpu.VMEM((tp - 1, rows + HALO, model), BF16),
            pltpu.VMEM((rows, model), BF16),
            pltpu.VMEM((tp - 1, rows + HALO, model), BF16),
            pltpu.VMEM(wq.shape, BF16),
            pltpu.VMEM(wk.shape, BF16),
            pltpu.VMEM(wv.shape, BF16),
            pltpu.VMEM(wo.shape, BF16),
            pltpu.VMEM(wout.shape, BF16),
            pltpu.VMEM((seq_len, 128), F32),
            pltpu.VMEM((HALO + seq_len, qk), F32),
            pltpu.VMEM((HALO + seq_len, qk), F32),
            pltpu.VMEM((seq_len, qk), BF16),
            pltpu.VMEM((seq_len, qk), BF16),
            pltpu.VMEM((seq_len, vd), BF16),
            pltpu.VMEM((seq_len, vd), BF16),
            pltpu.VMEM((seq_len, vd), F32),
            pltpu.VMEM((heads, seq_len, 128), F32),
            pltpu.VMEM((seq_len, vd), BF16),
            pltpu.VMEM((sp, piece, dv), BF16),
            pltpu.VMEM((sp, piece, dv), BF16),
            pltpu.VMEM((2, heads, dqk), F32),
            pltpu.VMEM((sp, 2, heads, dqk), F32),
            pltpu.VMEM((heads, dqk), F32),
            pltpu.VMEM((sp, heads, dqk), F32),
            pltpu.VMEM((sp, 2, heads, dqk), F32),
            pltpu.VMEM((sp, piece, dv), BF16),
            pltpu.VMEM((sp, piece, dv), BF16),
            pltpu.VMEM((tp - 1, chunks, rows, 512), BF16),
            pltpu.VMEM((tp - 1, chunks, rows, 512), BF16),
            dma((streams,)),
            dma,
            dma((7,)),
            dma((tp - 1,)),
            dma((tp - 1,)),
            dma((tp,)),
            dma,
        ]
        + [dma((sp,))] * 8
        + [dma((tp - 1, chunks))] * 2,
        compiler_params=pltpu.CompilerParams(
            collective_id=0, has_side_effects=True, vmem_limit_bytes=60 * 1024 * 1024
        ),
    )(
        tokens,
        norm_gain.reshape(1, model),
        wq,
        wk,
        wv,
        wo,
        wi.T,
        wf.T,
        cq,
        ck,
        offset,
        hgain.reshape(1, hgain.shape[0]),
        wout,
    )


def solution(mesh):
    in_specs = (
        P(("sp", "tp"), None),
        P(),
        P(None, "tp"),
        P(None, "tp"),
        P(None, "tp"),
        P(None, "tp"),
        P(),
        P(),
        P(),
        P(),
        P(None, "sp", "tp"),
        P(),
        P("tp", None),
    )
    out_specs = P(("sp", "tp"), None)
    step = functools.partial(body, mesh.shape["sp"], mesh.shape["tp"])
    return jax.shard_map(step, mesh=mesh, in_specs=in_specs, out_specs=out_specs, check_vma=False)
```

```python
import functools

import jax
import jax.numpy as jnp
from jax import lax
from jax.experimental import pallas as pl
from jax.experimental.pallas import tpu as pltpu
from jax.sharding import PartitionSpec as P

SPAN = 128
HALO = 16
EPS = 1e-06
EMPTY_LEVEL = -1e30
HIGHEST = lax.Precision.HIGHEST
MESH = pl.DeviceIdType.MESH
F32, BF16 = jnp.float32, jnp.bfloat16


def normalize(values, gain):
    widened = values.astype(F32)
    scaled = widened * lax.rsqrt(jnp.mean(widened * widened, axis=-1, keepdims=True) + EPS)
    return (scaled * gain).astype(BF16)


def dot_t(a, b):
    return lax.dot_general(a, b, (((1,), (1,)), ((), ())), preferred_element_type=F32)


def dot_tl(a, b):
    return lax.dot_general(a, b, (((0,), (0,)), ((), ())), preferred_element_type=F32)


def kernel(
    sp,
    tp,
    tokens_hbm,
    gain_hbm,
    wq_hbm,
    wk_hbm,
    wv_hbm,
    wo_hbm,
    wi_hbm,
    wf_hbm,
    cq_hbm,
    ck_hbm,
    offset_hbm,
    hgain_hbm,
    wout_hbm,
    out_ref,
    gain_ref,
    wi_ref,
    wf_ref,
    cq_ref,
    ck_ref,
    offset_ref,
    hgain_ref,
    ext_own,
    ext_oth,
    nor_own,
    nor_oth,
    wq,
    wk,
    wv,
    wo,
    wout,
    gcol,
    kpre,
    qpre,
    key,
    query,
    value,
    ogate,
    numer,
    cols,
    hidden,
    sbuf,
    rbuf,
    meta,
    mbuf,
    nmeta,
    nbuf,
    scales,
    pbuf,
    gbuf,
    sharesend,
    sharerecv,
    w_sem,
    t_sem,
    s_sem,
    tsend_sem,
    trecv_sem,
    hsend_sem,
    hrecv_sem,
    psend_sem,
    precv_sem,
    msend_sem,
    mrecv_sem,
    nsend_sem,
    nrecv_sem,
    gsend_sem,
    grecv_sem,
    osend_sem,
    orecv_sem,
):
    me = lax.axis_index("sp")
    core = lax.axis_index("tp")
    rows, model = tokens_hbm.shape
    seq_len = rows * tp
    blocks = seq_len // SPAN
    heads = offset_hbm.shape[2]
    dqk = wq.shape[1] // heads
    dv = wv.shape[1] // heads
    piece_rows = sbuf.shape[1]
    head_first = core * heads
    last = tp - 1

    barrier = pltpu.get_barrier_semaphore()

    def signal(to_sp, to_tp):
        pl.semaphore_signal(barrier, inc=1, device_id=(to_sp, to_tp), device_id_type=MESH)

    def greet(d, c):
        signal(lax.rem(me + d, sp), core)
        return c

    lax.fori_loop(1, sp, greet, 0)
    for d in range(1, tp):
        signal(me, lax.rem(core + d, tp))

    @pl.when(core == last)
    def _():
        for c in range(tp - 1):
            signal(lax.rem(me + 1, sp), c)

    @pl.when(core != last)
    def _():
        signal(lax.rem(me + sp - 1, sp), last)

    own_copy = pltpu.make_async_copy(tokens_hbm, ext_own, t_sem)
    own_copy.start()
    small = []
    for n, (src, dst) in enumerate(
        (
            (gain_hbm, gain_ref),
            (wi_hbm, wi_ref),
            (wf_hbm, wf_ref),
            (ck_hbm, ck_ref),
            (cq_hbm, cq_ref),
            (offset_hbm, offset_ref),
            (hgain_hbm, hgain_ref),
        )
    ):
        cp = pltpu.make_async_copy(src, dst, s_sem.at[n])
        cp.start()
        small.append(cp)
    streams = {}
    at = 0
    for name, hbm, vm in (
        ("v", wv_hbm, wv),
        ("k", wk_hbm, wk),
        ("q", wq_hbm, wq),
        ("o", wo_hbm, wo),
        ("out", wout_hbm, wout),
    ):
        streams[name] = []
        for c in range(0, hbm.shape[1], 512):
            cp = pltpu.make_async_copy(
                hbm.at[:, pl.ds(c, 512)], vm.at[:, pl.ds(c, 512)], w_sem.at[at]
            )
            cp.start()
            streams[name].append(cp)
            at += 1

    for cp in small:
        cp.wait()
    own_copy.wait()
    gain = gain_ref[...]
    nor_own[...] = normalize(ext_own[...], gain)
    own = pl.ds(pl.multiple_of(core * rows, 16), rows)
    gate_weights = jnp.concatenate(
        [
            wi_ref[...].astype(F32),
            wf_ref[...].astype(F32),
            jnp.zeros((128 - 2 * wi_ref.shape[0], model), F32),
        ],
        axis=0,
    ).astype(BF16)
    gcol[own, :] = dot_t(nor_own[...], gate_weights)

    pl.semaphore_wait(barrier, sp - 1 + tp - 1 + jnp.where(core == last, tp - 1, 1))

    def token_copy(d, target, source):
        return pltpu.make_async_remote_copy(
            src_ref=ext_own,
            dst_ref=ext_oth.at[d - 1, pl.ds(0, rows)],
            send_sem=tsend_sem.at[d - 1],
            recv_sem=trecv_sem.at[d - 1],
            device_id=(me, target),
            device_id_type=MESH,
        )

    def halo_copy(c):
        return pltpu.make_async_remote_copy(
            src_ref=ext_own.at[pl.ds(rows - HALO, HALO)],
            dst_ref=ext_oth.at[tp - 2, pl.ds(rows, HALO)],
            send_sem=hsend_sem.at[c],
            recv_sem=hrecv_sem,
            device_id=(lax.rem(me + 1, sp), c),
            device_id_type=MESH,
        )

    sends_halo = jnp.logical_and(core == last, me < sp - 1)

    @pl.when(sends_halo)
    def _():
        for c in range(tp):
            halo_copy(c).start()

    for d in range(1, tp):
        token_copy(d, lax.rem(core + d, tp), None).start()

    def project(w, lhs, n):
        return jnp.dot(lhs, w[:, n : n + 256], preferred_element_type=F32).astype(BF16)

    qk, vd = wq.shape[1], wv.shape[1]
    pre_own = pl.ds(pl.multiple_of(HALO + core * rows, 16), rows)

    for c, cp in enumerate(streams["v"]):
        cp.wait()
        for n in range(c * 512, c * 512 + 512, 256):
            value[own, n : n + 256] = project(wv, nor_own[...], n)
    for cp in streams["k"]:
        cp.wait()
    for n in range(0, qk, 256):
        kpre[pre_own, n : n + 256] = project(wk, nor_own[...], n).astype(F32)

    @pl.when(sends_halo)
    def _():
        for c in range(tp):
            halo_copy(c).wait_send()

    for d in range(1, tp):
        cp = token_copy(d, lax.rem(core + d, tp), None)
        cp.wait_send()
        cp.wait_recv()
    for d in range(1, tp):
        nor_oth[d - 1, pl.ds(0, rows), :] = normalize(ext_oth[d - 1, pl.ds(0, rows), :], gain)

    def place(d):
        return lax.rem(core + tp - d, tp) * rows

    for d in range(1, tp):
        gcol[pl.ds(pl.multiple_of(place(d), 16), rows), :] = dot_t(
            nor_oth[d - 1, pl.ds(0, rows), :], gate_weights
        )

    gates_all = jnp.concatenate(
        [gcol[b * SPAN : (b + 1) * SPAN, :].T for b in range(blocks)], axis=1
    )
    total_heads = wi_ref.shape[0]
    in_rows = gates_all[:heads]
    fo_rows = gates_all[total_heads : total_heads + heads]
    for c in range(1, tp):
        in_rows = jnp.where(core == c, gates_all[c * heads : (c + 1) * heads], in_rows)
        fo_rows = jnp.where(
            core == c,
            gates_all[total_heads + c * heads : total_heads + (c + 1) * heads],
            fo_rows,
        )
    head_id = lax.broadcasted_iota(jnp.int32, (heads, SPAN), 0)

    def offsets(kind, b):
        spread = jnp.zeros((heads, SPAN), F32)
        for h in range(heads):
            spread = jnp.where(head_id == h, offset_ref[b, kind : kind + 1, h : h + 1], spread)
        return spread

    upper = (
        lax.broadcasted_iota(jnp.int32, (SPAN, SPAN), 0)
        <= lax.broadcasted_iota(jnp.int32, (SPAN, SPAN), 1)
    ).astype(F32)
    gate, cum, tot = [], [], []
    for b in range(blocks):
        part = slice(b * SPAN, (b + 1) * SPAN)
        gate.append(in_rows[:, part] + offsets(0, b))
        x = fo_rows[:, part] + offsets(1, b)
        lf = jnp.minimum(x, 0.0) - jnp.log1p(jnp.exp(-jnp.abs(x)))
        lf8 = jnp.concatenate([lf, jnp.zeros((8 - heads, SPAN), F32)], axis=0) if heads < 8 else lf
        c = jnp.dot(lf8, upper, precision=HIGHEST, preferred_element_type=F32)[:heads]
        cum.append(c)
        tot.append(c[:, SPAN - 1 :])
    base = [jnp.zeros((heads, 1), F32)]
    for b in range(blocks):
        base.append(base[-1] + tot[b])
    tail = [None] * blocks
    acc = jnp.zeros((heads, 1), F32)
    for b in reversed(range(blocks)):
        tail[b] = acc
        acc = acc + tot[b]
    wlog = [tail[b] + (tot[b] - cum[b]) + gate[b] for b in range(blocks)]
    level = jnp.max(wlog[0], axis=1, keepdims=True)
    for b in range(1, blocks):
        level = jnp.maximum(level, jnp.max(wlog[b], axis=1, keepdims=True))
    wrows = [jnp.exp(w - level) for w in wlog]
    stacked = [jnp.concatenate([cum[b], wrows[b]], axis=0).T for b in range(blocks)]

    def to_peer(src, dst, ssem, rsem, target):
        return pltpu.make_async_remote_copy(
            src_ref=src,
            dst_ref=dst,
            send_sem=ssem,
            recv_sem=rsem,
            device_id=(target, core),
            device_id_type=MESH,
        )

    def meta_copy(source, target):
        return to_peer(meta, mbuf.at[source], msend_sem.at[target], mrecv_sem.at[source], target)

    def norm_copy(source, target):
        return to_peer(nmeta, nbuf.at[source], nsend_sem.at[target], nrecv_sem.at[source], target)

    def piece_copy(source, target):
        return to_peer(
            sbuf.at[target], rbuf.at[source], psend_sem.at[target], precv_sem.at[source], target
        )

    def prefix_copy(source, target):
        return to_peer(
            pbuf.at[target], gbuf.at[source], gsend_sem.at[target], grecv_sem.at[source], target
        )

    meta[0] = jnp.broadcast_to(base[blocks], (heads, dqk))
    meta[1] = jnp.broadcast_to(level, (heads, dqk))

    for n in range(0, vd, 256):
        for d in range(1, tp):
            value[pl.ds(pl.multiple_of(place(d), 16), rows), n : n + 256] = project(
                wv, nor_oth[d - 1, pl.ds(0, rows), :], n
            )

    def send_meta(d, c):
        meta_copy(me, lax.rem(me + d, sp)).start()
        return c

    lax.fori_loop(1, sp, send_meta, 0)
    mbuf[me] = meta[...]

    @pl.when(me > 0)
    def _():
        halo_copy(core).wait_recv()

    @pl.when(me == 0)
    def _():
        ext_oth[tp - 2, pl.ds(rows, HALO), :] = jnp.zeros((HALO, model), BF16)

    nor_oth[tp - 2, pl.ds(rows, HALO), :] = normalize(ext_oth[tp - 2, pl.ds(rows, HALO), :], gain)

    def rest_of(pre, w, n):
        for d in range(1, tp):
            more = HALO if d == tp - 1 else 0
            got = project(w, nor_oth[d - 1, pl.ds(0, rows + more), :], n).astype(F32)
            pre[pl.ds(pl.multiple_of(HALO + place(d), 16), rows), n : n + 256] = got[:rows]
            if more:
                pre[pl.ds(0, HALO), n : n + 256] = got[rows:]

    def mix(pre, taps_ref, dest, scale, n):
        taps = taps_ref[:, pl.ds(pl.multiple_of(core * qk + n, 128), 128)].astype(F32)
        count = taps.shape[0]
        mixed = jnp.zeros((seq_len, 128), F32)
        for j in range(count):
            mixed = (
                mixed
                + taps[j : j + 1, :] * pre[pl.ds(HALO - count + 1 + j, seq_len), n : n + 128]
            )
        dest[:, n : n + 128] = (mixed * jax.nn.sigmoid(mixed) * scale).astype(BF16)

    per = sp // heads
    for h in range(heads):
        if (h * dqk) % 256 == 0:
            rest_of(kpre, wk, h * dqk)
        mix(kpre, ck_ref, key, dqk**-0.5, h * dqk)
        weighted = [
            stacked[b][:, heads + h : heads + h + 1]
            * key[b * SPAN : (b + 1) * SPAN, h * dqk : (h + 1) * dqk].astype(F32)
            for b in range(blocks)
        ]
        norm = jnp.sum(weighted[0], axis=0, keepdims=True)
        for b in range(1, blocks):
            norm = norm + jnp.sum(weighted[b], axis=0, keepdims=True)
        state = dot_tl(
            jnp.concatenate([w.astype(BF16) for w in weighted], axis=0),
            value[:, h * dv : (h + 1) * dv],
        )
        for p in range(per):
            sbuf[p * heads + h] = state[p * piece_rows : (p + 1) * piece_rows].astype(BF16)
        nmeta[h : h + 1, :] = norm
        for p in range(per):
            target = p * heads + h

            @pl.when(me != target)
            def _():
                piece_copy(me, target).start()

            @pl.when(me == target)
            def _():
                rbuf[target] = sbuf[target]

    def send_norm(d, c):
        norm_copy(me, lax.rem(me + d, sp)).start()
        return c

    lax.fori_loop(1, sp, send_norm, 0)
    nbuf[me] = nmeta[...]

    for cp in streams["q"]:
        cp.wait()
    for n in range(0, qk, 256):
        qpre[pre_own, n : n + 256] = project(wq, nor_own[...], n).astype(F32)
        rest_of(qpre, wq, n)
        for m in range(n, n + 256, 128):
            mix(qpre, cq_ref, query, 1.0, m)

    my_head = lax.rem(me, heads)
    small_id = lax.broadcasted_iota(jnp.int32, (heads, dqk), 0)

    def weigh(i, carry):
        lev, lev_in = carry
        j = i - 1

        @pl.when(j != me)
        def _():
            meta_copy(j, me).wait_recv()

        shifted = lev + mbuf[j, 0]
        new_lev = jnp.maximum(shifted, mbuf[j, 1])
        one, two = jnp.exp(shifted - new_lev), jnp.exp(mbuf[j, 1] - new_lev)
        scales[i, 0] = one
        scales[i, 1] = two
        return new_lev, jnp.where(i == me, new_lev, lev_in)

    empty = jnp.full((heads, dqk), EMPTY_LEVEL, F32)
    _, lev_in = lax.fori_loop(1, sp, weigh, (empty, empty))

    causal = lax.broadcasted_iota(jnp.int32, (SPAN, SPAN), 0) >= lax.broadcasted_iota(
        jnp.int32, (SPAN, SPAN), 1
    )

    def intra(h):
        for i in range(blocks):
            col = stacked[i][:, h : h + 1]
            logs = []
            top = None
            for j in range(i + 1):
                row = (gate[j][h : h + 1] - cum[j][h : h + 1]) + (
                    base[i][h : h + 1] - base[j][h : h + 1]
                )
                tile = col + row
                if j == i:
                    tile = jnp.where(causal, tile, -jnp.inf)
                logs.append(tile)
                t = jnp.max(tile, axis=1, keepdims=True)
                top = t if top is None else jnp.maximum(top, t)
            q = query[i * SPAN : (i + 1) * SPAN, h * dqk : (h + 1) * dqk]
            den = jnp.zeros((SPAN, 1), F32)
            num = jnp.zeros((SPAN, dv), F32)
            for j in range(i + 1):
                k = key[j * SPAN : (j + 1) * SPAN, h * dqk : (h + 1) * dqk]
                scores = dot_t(q, k) * jnp.exp(logs[j] - top)
                den = den + jnp.sum(scores, axis=1, keepdims=True)
                num = num + jnp.dot(
                    scores.astype(BF16),
                    value[j * SPAN : (j + 1) * SPAN, h * dv : (h + 1) * dv],
                    preferred_element_type=F32,
                )
            numer[i * SPAN : (i + 1) * SPAN, h * dv : (h + 1) * dv] = num
            cols[h, i * SPAN : (i + 1) * SPAN, 0:1] = den
            cols[h, i * SPAN : (i + 1) * SPAN, 1:2] = top

    for h in range(heads // 2):
        intra(h)

    def pick(x):
        r = jnp.sum(jnp.where(small_id == my_head, x, 0.0), axis=0, keepdims=True)
        return jnp.concatenate([r] * (dv // dqk), axis=1)

    def combine(i, piece):
        j = i - 1
        one, two = pick(scales[i, 0]), pick(scales[i, 1])

        @pl.when(j != me)
        def _():
            piece_copy(j, me).wait_recv()

        piece = one * piece + two * rbuf[j].astype(F32)
        pbuf[i] = piece.astype(BF16)

        @pl.when(i == me)
        def _():
            gbuf[me] = piece.astype(BF16)

        @pl.when(jnp.logical_and(i > 1, j != me))
        def _():
            prefix_copy(me, j).start()

        return piece

    lax.fori_loop(1, sp, combine, jnp.zeros((piece_rows, dv), F32))

    @pl.when(me != sp - 1)
    def _():
        prefix_copy(me, sp - 1).start()

    for h in range(heads // 2, heads):
        intra(h)

    for c, cp in enumerate(streams["o"]):
        cp.wait()
        for n in range(c * 512, c * 512 + 512, 256):
            ogate[own, n : n + 256] = project(wo, nor_own[...], n)
            for d in range(1, tp):
                ogate[pl.ds(pl.multiple_of(place(d), 16), rows), n : n + 256] = project(
                    wo, nor_oth[d - 1, pl.ds(0, rows), :], n
                )

    @pl.when(me != sp - 1)
    def _():
        meta_copy(sp - 1, me).wait_recv()
        piece_copy(sp - 1, me).wait_recv()

    def take_norm(d, c):
        norm_copy(lax.rem(me + d, sp), me).wait_recv()
        return c

    lax.fori_loop(1, sp, take_norm, 0)
    nor_in = lax.fori_loop(
        1,
        me + 1,
        lambda i, nor: scales[i, 0] * nor + scales[i, 1] * nbuf[i - 1],
        jnp.zeros((heads, dqk), F32),
    )

    @pl.when(me == 0)
    def _():
        gbuf[...] = jnp.zeros(gbuf.shape, BF16)

    for h in range(heads):
        for p in range(per):
            source = p * heads + h

            @pl.when(jnp.logical_and(me > 0, me != source))
            def _():
                prefix_copy(source, me).wait_recv()

        state = jnp.concatenate([gbuf[p * heads + h] for p in range(per)], axis=0)
        hgain = hgain_ref[:, pl.ds(pl.multiple_of((head_first + h) * dv, 128), dv)]
        for i in range(blocks):
            part = slice(i * SPAN, (i + 1) * SPAN)
            q = query[part, h * dqk : (h + 1) * dqk]
            carried = (stacked[i][:, h : h + 1] + base[i][h : h + 1]) + lev_in[h : h + 1, 0:1]
            den, own_top = cols[h, part, 0:1], cols[h, part, 1:2]
            top = jnp.maximum(own_top, carried)
            new, old = jnp.exp(own_top - top), jnp.exp(carried - top)
            from_norm = jnp.sum(q.astype(F32) * nor_in[h : h + 1], axis=1, keepdims=True)
            den = new * den + old * from_norm
            num = new * numer[part, h * dv : (h + 1) * dv] + old * jnp.dot(
                q, state, preferred_element_type=F32
            )
            cell = num / jnp.maximum(jnp.abs(den), jnp.exp(-top))
            cell = cell * lax.rsqrt(jnp.mean(cell * cell, axis=-1, keepdims=True) + EPS)
            hidden[part, h * dv : (h + 1) * dv] = (
                cell * hgain * jax.nn.sigmoid(ogate[part, h * dv : (h + 1) * dv].astype(F32))
            ).astype(BF16)

    sends = []
    chunks = len(streams["out"])
    for c, cp in enumerate(streams["out"]):
        cp.wait()
    for d in range(1, tp):
        target = lax.rem(core + d, tp)
        theirs = pl.ds(pl.multiple_of(target * rows, 16), rows)
        for c in range(chunks):
            sharesend[d - 1, c] = jnp.dot(
                hidden[theirs, :], wout[:, c * 512 : (c + 1) * 512], preferred_element_type=F32
            ).astype(BF16)
            cp = pltpu.make_async_remote_copy(
                src_ref=sharesend.at[d - 1, c],
                dst_ref=sharerecv.at[d - 1, c],
                send_sem=osend_sem.at[d - 1, c],
                recv_sem=orecv_sem.at[d - 1, c],
                device_id=(me, target),
                device_id_type=MESH,
            )
            cp.start()
            sends.append(cp)
    for c in range(chunks):
        total = jnp.dot(
            hidden[own, :], wout[:, c * 512 : (c + 1) * 512], preferred_element_type=F32
        )
        for d in range(1, tp):
            sends[(d - 1) * chunks + c].wait_recv()
            total = total + sharerecv[d - 1, c].astype(F32)
        out_ref[:, c * 512 : (c + 1) * 512] = total.astype(BF16)

    for cp in sends:
        cp.wait_send()

    def settle(d, c):
        target = lax.rem(me + d, sp)
        meta_copy(me, target).wait_send()
        norm_copy(me, target).wait_send()
        piece_copy(me, target).wait_send()

        @pl.when(target > 0)
        def _():
            prefix_copy(me, target).wait_send()

        return c

    lax.fori_loop(1, sp, settle, 0)


def body(sp, tp, tokens, norm_gain, wq, wk, wv, wo, wi, wf, cq, ck, offset, hgain, wout):
    rows, model = tokens.shape
    seq_len = rows * tp
    heads = offset.shape[2]
    qk, vd = wq.shape[1], wv.shape[1]
    dqk, dv = qk // heads, vd // heads
    piece = qk // sp
    chunks = wout.shape[1] // 512
    streams = (2 * qk + 2 * vd + wout.shape[1]) // 512
    hbm = pl.BlockSpec(memory_space=pltpu.HBM)
    vmem = pl.BlockSpec(memory_space=pltpu.VMEM)
    dma = pltpu.SemaphoreType.DMA
    return pl.pallas_call(
        functools.partial(kernel, sp, tp),
        out_shape=pltpu.VMEM((rows, wout.shape[1]), BF16),
        in_specs=[hbm] * 13,
        out_specs=vmem,
        scratch_shapes=[
            pltpu.VMEM((1, model), F32),
            pltpu.VMEM((wi.shape[1], model), BF16),
            pltpu.VMEM((wf.shape[1], model), BF16),
            pltpu.VMEM(cq.shape, BF16),
            pltpu.VMEM(ck.shape, BF16),
            pltpu.VMEM((offset.shape[1], offset.shape[0], heads), F32),
            pltpu.VMEM((1, hgain.shape[0]), F32),
            pltpu.VMEM((rows, model), BF16),
            pltpu.VMEM((tp - 1, rows + HALO, model), BF16),
            pltpu.VMEM((rows, model), BF16),
            pltpu.VMEM((tp - 1, rows + HALO, model), BF16),
            pltpu.VMEM(wq.shape, BF16),
            pltpu.VMEM(wk.shape, BF16),
            pltpu.VMEM(wv.shape, BF16),
            pltpu.VMEM(wo.shape, BF16),
            pltpu.VMEM(wout.shape, BF16),
            pltpu.VMEM((seq_len, 128), F32),
            pltpu.VMEM((HALO + seq_len, qk), F32),
            pltpu.VMEM((HALO + seq_len, qk), F32),
            pltpu.VMEM((seq_len, qk), BF16),
            pltpu.VMEM((seq_len, qk), BF16),
            pltpu.VMEM((seq_len, vd), BF16),
            pltpu.VMEM((seq_len, vd), BF16),
            pltpu.VMEM((seq_len, vd), F32),
            pltpu.VMEM((heads, seq_len, 128), F32),
            pltpu.VMEM((seq_len, vd), BF16),
            pltpu.VMEM((sp, piece, dv), BF16),
            pltpu.VMEM((sp, piece, dv), BF16),
            pltpu.VMEM((2, heads, dqk), F32),
            pltpu.VMEM((sp, 2, heads, dqk), F32),
            pltpu.VMEM((heads, dqk), F32),
            pltpu.VMEM((sp, heads, dqk), F32),
            pltpu.VMEM((sp, 2, heads, dqk), F32),
            pltpu.VMEM((sp, piece, dv), BF16),
            pltpu.VMEM((sp, piece, dv), BF16),
            pltpu.VMEM((tp - 1, chunks, rows, 512), BF16),
            pltpu.VMEM((tp - 1, chunks, rows, 512), BF16),
            dma((streams,)),
            dma,
            dma((7,)),
            dma((tp - 1,)),
            dma((tp - 1,)),
            dma((tp,)),
            dma,
        ]
        + [dma((sp,))] * 8
        + [dma((tp - 1, chunks))] * 2,
        compiler_params=pltpu.CompilerParams(
            collective_id=0, has_side_effects=True, vmem_limit_bytes=60 * 1024 * 1024
        ),
    )(
        tokens,
        norm_gain.reshape(1, model),
        wq,
        wk,
        wv,
        wo,
        wi.T,
        wf.T,
        cq,
        ck,
        jnp.transpose(offset, (1, 0, 2)),
        hgain.reshape(1, hgain.shape[0]),
        wout,
    )


def solution(mesh):
    in_specs = (
        P(("sp", "tp"), None),
        P(),
        P(None, "tp"),
        P(None, "tp"),
        P(None, "tp"),
        P(None, "tp"),
        P(),
        P(),
        P(),
        P(),
        P(None, "sp", "tp"),
        P(),
        P("tp", None),
    )
    out_specs = P(("sp", "tp"), None)
    step = functools.partial(body, mesh.shape["sp"], mesh.shape["tp"])
    return jax.shard_map(step, mesh=mesh, in_specs=in_specs, out_specs=out_specs, check_vma=False)
```
